32 devices in a mesh: ep: 16 (over z, y, x), tp: 2 (over core).
Axes of the slice: x: 2, y: 2, z: 4, core: 2. Of those that a mesh axis runs over, the one named last changes fastest.
Arguments:
- tokens: bfloat16 [8192, 2048], P(('ep', 'tp')), may hold values from -6 to 6
- norm_gain: float32 [2048], replicated, may hold values from 0.1 to 1.9
- expert_ids: int32 [8192, 2], P(('ep', 'tp')), may hold values from 0 to 15, all different within a row; in each aligned block of 256 rows (0 to 255, 256 to 511, ...) at most 48 rows name the same one
- route_weights: float32 [8192, 2], P(('ep', 'tp')), may hold values from 0.2 to 1.2
- expert_gate: bfloat16 [16, 2048, 512], P('ep', None, 'tp'), may hold values from -0.125 to 0.125
- expert_up: bfloat16 [16, 2048, 512], P('ep', None, 'tp'), may hold values from -0.125 to 0.125
- expert_down: bfloat16 [16, 512, 2048], P('ep', 'tp'), may hold values from -0.25 to 0.25
- shared_gate: bfloat16 [2048, 512], P(None, 'tp'), may hold values from -0.125 to 0.125
- shared_up: bfloat16 [2048, 512], P(None, 'tp'), may hold values from -0.125 to 0.125
- shared_down: bfloat16 [512, 2048], P('tp'), may hold values from -0.25 to 0.25
Outputs:
- mixed: bfloat16 [8192, 2048], P(('ep', 'tp'))
The draws below stay inside these ranges and needn't reach their ends.
Inputs may be any that keep to these rules, and one draw needn't show every extreme that they name: `expert_ids`: each token names 2 different experts. Among the tokens of one device (aligned blocks of 256 rows) no expert is named by more than 48 tokens, and in every block some expert is named by exactly 48.
All inputs are finite; a program needn't handle non-finite values.
Results may differ from the reference program's by a relative error of at most 0.0075.
Values may be sent and summed in bfloat16 or wider, within the bound.
No kernel may reach another device: no remote copies, remote signals or barrier semaphores. Data moves between devices by JAX's collectives and lax.ppermute only.
A program may use at most 64 MiB of HBM per device.

```python
import math
import jax
import jax.numpy as jnp
import numpy as np
from jax import lax

D = 2048
DE = 512
DS = 512
TOP_K = 2
TOK_DEV = 256
EXPERTS = 16
CAP = 48
TOKENS = 8192
N_EP = 16
N_TP = 2


def block_scale(key, shape, pieces, smallest, top_value):
    factor_of, own = 1.0, jax.random.fold_in(key, 6)
    for axis_at, blocks in pieces:
        draws = jnp.exp(jax.random.uniform(jax.random.fold_in(own, axis_at), (blocks,), jnp.float32, smallest / len(pieces), top_value / len(pieces)))
        factor_of = factor_of * jnp.repeat(draws, shape[axis_at] // blocks).reshape([-1 if axis == axis_at else 1 for axis in range(len(shape))])
    return factor_of


def assign_block(key, own, number, rows, amount, top, most, skew):
    order = jax.random.permutation(key, amount)
    heavy_load, ordinary = load_shares(amount, rows * top, most, skew, True), load_shares(amount, rows * top, most, skew, False)
    places = jnp.arange(amount)

    def named(lengths, offset_by):
        used = int((lengths > 0).sum())
        fixed = max(1, used // 4)
        moved = fixed + (places - fixed + offset_by * (used - fixed)) % max(1, amount - fixed)
        return jnp.zeros((amount,), jnp.int32).at[order[jnp.where(places < fixed, places, moved)]].set(jnp.asarray(lengths, jnp.int32))

    lengths = jnp.where(number % 4 == 0, named(heavy_load, number // 4), named(ordinary, number - number // 4 - 1))
    mixed = jax.random.permutation(jax.random.fold_in(own, 3), amount)
    giver, sink = mixed[0:amount // 2 * 2:2], mixed[1:amount // 2 * 2:2]
    slack = jnp.minimum(lengths[giver] - 1, most - lengths[sink]) // 2
    slack = jnp.where((giver == order[0]) | (sink == order[0]) | (lengths[sink] == 0), 0, jnp.maximum(slack, 0))
    moved = jax.random.randint(jax.random.fold_in(own, 4), (amount // 2,), 0, 1 << 20) % (slack + 1)
    lengths = lengths.at[giver].add(-moved).at[sink].add(moved)
    items = jnp.searchsorted(jnp.cumsum(lengths), jnp.arange(rows * top), side="right").astype(jnp.int32)
    grid = items.reshape(top, rows).T
    grid = grid[jax.random.permutation(jax.random.fold_in(own, 1), rows)]
    offset_by = jax.random.randint(jax.random.fold_in(own, 2), (rows, 1), 0, top)
    return jnp.take_along_axis(grid, (jnp.arange(top)[None, :] + offset_by) % top, axis=1)


def load_shares(number_of, total, limit, skew, full):
    portions = [(1 << 20) // math.isqrt(standing ** skew) + 1 for standing in range(1, number_of + 1)]
    largest = limit if full else min(limit, max(-(-total // number_of), total * portions[0] // sum(portions)))
    least = 1 if total - largest >= number_of - 1 else 0
    holding, spare = [largest] + [least] * (number_of - 1), total - largest - least * (number_of - 1)
    while spare > 0:
        movable = [i for i in range(1, number_of) if holding[i] < largest] or [i for i in range(1, number_of) if holding[i] < limit]
        mass, left = sum([portions[i] for i in movable]), spare
        for i in movable:
            addition = min(limit - holding[i], max(1, left * portions[i] // mass), spare)
            holding[i] = holding[i] + addition
            spare = spare - addition
    return np.array(holding)


def noise(own_key, extent, spread, reach, split=(), kind=jnp.bfloat16):
    gain = block_scale(own_key, extent, split, -0.22, 0.18) if split else 1.0
    array = jax.random.normal(own_key, extent, jnp.float32) * spread * gain
    return jnp.minimum(jnp.maximum(array, -reach), reach).astype(kind)


def setup_inputs(seed: int = 0) -> dict:
    key_of = jax.random.split(jax.random.key(seed), 11)
    tokens = noise(key_of[0], (TOKENS, D), 1.0, 6.0, ((0, 32),))
    norm_gain = jnp.clip(1.0 + 0.18 * jax.random.normal(key_of[1], (D,), jnp.float32), 0.1, 1.9)
    expert_ids_keys = jax.random.split(jax.random.fold_in(key_of[2], 1), TOKENS // TOK_DEV)
    expert_ids_turns = jax.random.permutation(jax.random.fold_in(key_of[2], 3), TOKENS // TOK_DEV)
    expert_ids = jax.vmap(lambda own, number: assign_block(jax.random.fold_in(key_of[2], 2), own, number, TOK_DEV, EXPERTS, TOP_K, CAP, 2))(expert_ids_keys, expert_ids_turns).reshape((TOKENS, TOP_K))
    route_weights = jnp.clip(0.2 + 1 * jax.random.uniform(key_of[3], (TOKENS, TOP_K), jnp.float32) ** block_scale(key_of[3], (TOKENS, TOP_K), ((0, 32),), -0.2, 0.2), 0.2, 1.2)
    expert_gate = noise(key_of[4], (EXPERTS, D, DE), D ** -0.5, 0.125, ((0, 16), (2, 2)))
    expert_up = noise(key_of[5], (EXPERTS, D, DE), D ** -0.5, 0.125, ((0, 16), (2, 2)))
    expert_down = noise(key_of[6], (EXPERTS, DE, D), DE ** -0.5, 0.25, ((0, 16), (1, 2)))
    shared_gate = noise(key_of[7], (D, DS), D ** -0.5, 0.125, ((1, 2),))
    shared_up = noise(key_of[8], (D, DS), D ** -0.5, 0.125, ((1, 2),))
    shared_down = noise(key_of[9], (DS, D), DS ** -0.5, 0.25, ((0, 2),))
    return {"tokens": tokens, "norm_gain": norm_gain, "expert_ids": expert_ids, "route_weights": route_weights, "expert_gate": expert_gate, "expert_up": expert_up, "expert_down": expert_down, "shared_gate": shared_gate, "shared_up": shared_up, "shared_down": shared_down}


epsilon = 1e-06

def normalize(tokens, norm_gain):
    values = tokens.astype(jnp.float32)
    factor = lax.rsqrt(lax.optimization_barrier(jnp.mean(values * values, axis=1, keepdims=True)) + epsilon)
    return (values * factor * norm_gain[None, :]).astype(jnp.bfloat16)

def halves(row_block, gate_w, up_w, down_w):
    half_width = gate_w.shape[1] // N_TP
    summed = jnp.zeros((row_block.shape[0], down_w.shape[1]), jnp.float32)
    for portion in range(N_TP):
        first = portion * half_width
        gate_value = jnp.dot(row_block, gate_w[:, first:first + half_width], preferred_element_type=jnp.float32)
        up_value = jnp.dot(row_block, up_w[:, first:first + half_width], preferred_element_type=jnp.float32)
        hidden = (jax.nn.silu(gate_value) * up_value).astype(jnp.bfloat16)
        partial_value = jnp.dot(hidden, down_w[first:first + half_width], preferred_element_type=jnp.float32)
        rounded = lax.optimization_barrier(partial_value.astype(jnp.bfloat16))
        summed = summed + rounded.astype(jnp.float32)
    return summed

def reference(tokens, norm_gain, expert_ids, route_weights, expert_gate, expert_up, expert_down, shared_gate, shared_up, shared_down):
    normed = normalize(tokens, norm_gain)
    total_rows = tokens.shape[0]
    shared_out = halves(normed, shared_gate, shared_up, shared_down)
    flat_ids = expert_ids.reshape(-1).astype(jnp.int32)
    assigned = flat_ids.shape[0]
    ordering = jnp.argsort(flat_ids, stable=True).astype(jnp.int32)
    counts = jnp.bincount(flat_ids, length=EXPERTS).astype(jnp.int32)
    starts = (jnp.cumsum(counts) - counts).astype(jnp.int32)
    most_rows = N_EP * N_TP * CAP
    padded = jnp.concatenate([normed, jnp.zeros((1, D), jnp.bfloat16)], axis=0)
    flat_weights = route_weights.reshape(-1)

    def per_expert(totals, expert):
        slot_range = jnp.arange(most_rows, dtype=jnp.int32)
        filled = slot_range < counts[expert]
        row_index = jnp.minimum(starts[expert] + slot_range, assigned - 1)
        assign = jnp.where(filled, ordering[row_index], assigned)
        token_index = (assign // TOP_K).astype(jnp.int32)
        row_block = padded[token_index]
        expert_out = halves(row_block, expert_gate[expert], expert_up[expert], expert_down[expert]).astype(jnp.bfloat16)
        weight_rows = jnp.where(filled, flat_weights[jnp.minimum(assign, assigned - 1)], jnp.float32(0.0))
        totals = totals.at[token_index].add(expert_out.astype(jnp.float32) * weight_rows[:, None])
        return (totals, None)
    totals, _ = lax.scan(per_expert, jnp.zeros((total_rows + 1, D), jnp.float32), jnp.arange(EXPERTS, dtype=jnp.int32))
    routed = totals[:total_rows]
    return (routed + shared_out).astype(jnp.bfloat16)
```

```python
import jax
import jax.numpy as jnp
from jax import lax
from jax.sharding import PartitionSpec as P

epsilon = 1e-06


def normalize(tokens, norm_gain):
    values = tokens.astype(jnp.float32)
    factor = lax.rsqrt(jnp.mean(values * values, axis=1, keepdims=True) + epsilon)
    return (values * factor * norm_gain[None, :]).astype(jnp.bfloat16)


def dot(left, right):
    return jnp.dot(left, right, preferred_element_type=jnp.float32)


def swap_cores(array):
    size = lax.axis_size("tp")
    return lax.ppermute(array, "tp", [(i, (i + 1) % size) for i in range(size)])


def hidden_units(rows, gate_w, up_w):
    return (jax.nn.silu(dot(rows, gate_w)) * dot(rows, up_w)).astype(jnp.bfloat16)


def feed_forward(rows, halves):
    summed = 0.0
    for gate_w, up_w, down_w in halves:
        summed = summed + dot(hidden_units(rows, gate_w, up_w), down_w)
    return summed


def slot_masks(ids, weights, experts, capacity):
    rows = ids.shape[0]
    numbers = jnp.arange(experts, dtype=jnp.int32)
    named = ids.T[:, None, :] == numbers[None, :, None]
    member = jnp.any(named, axis=0)
    weight = jnp.sum(jnp.where(named, weights.T[:, None, :], 0.0), axis=0)
    places = jnp.arange(rows)
    earlier = (places[:, None] < places[None, :]).astype(jnp.bfloat16)
    rank = dot(member.astype(jnp.bfloat16), earlier).astype(jnp.int32)
    rank = jnp.where(member, rank, -1)
    chosen = rank[:, None, :] == jnp.arange(capacity, dtype=jnp.int32)[None, :, None]
    pick = chosen.astype(jnp.bfloat16).reshape(experts * capacity, rows)
    scaled = jnp.where(chosen, weight[:, None, :], 0.0).reshape(experts * capacity, rows)
    return pick, scaled


def combine(scaled, results):
    high = lax.reduce_precision(scaled, 8, 7)
    low = (scaled - high).astype(jnp.bfloat16)
    dims = (((0,), (0,)), ((), ()))
    return lax.dot_general(
        high.astype(jnp.bfloat16), results, dims, preferred_element_type=jnp.float32
    ) + lax.dot_general(low, results, dims, preferred_element_type=jnp.float32)


def body(
    tokens,
    norm_gain,
    expert_ids,
    route_weights,
    expert_gate,
    expert_up,
    expert_down,
    shared_gate,
    shared_up,
    shared_down,
):
    tok_rows, model_width = tokens.shape
    ep_size = lax.axis_size("ep")
    experts = expert_gate.shape[0] * ep_size
    capacity = 3 * tok_rows * expert_ids.shape[1] // (2 * experts)
    normed = normalize(tokens, norm_gain)
    own = (expert_gate[0], expert_up[0], expert_down[0])
    shared = (shared_gate, shared_up, shared_down)
    routed_halves = (own, tuple(swap_cores(w) for w in own))
    shared_halves = (shared, tuple(swap_cores(w) for w in shared))
    pick, scaled = slot_masks(expert_ids, route_weights, experts, capacity)
    outgoing = dot(pick, normed).astype(jnp.bfloat16)
    received = lax.all_to_all(
        outgoing.reshape(ep_size, capacity, model_width), "ep", 0, 0, tiled=True
    )
    results = feed_forward(
        received.reshape(ep_size * capacity, model_width), routed_halves
    ).astype(jnp.bfloat16)
    returned = lax.all_to_all(
        results.reshape(ep_size, capacity, model_width), "ep", 0, 0, tiled=True
    )
    shared_out = feed_forward(normed, shared_halves)
    routed = combine(scaled, returned.reshape(experts * capacity, model_width))
    return (routed + shared_out).astype(jnp.bfloat16)


def solution(mesh):
    placed = (
        P(("ep", "tp"), None),
        P(),
        P(("ep", "tp"), None),
        P(("ep", "tp"), None),
        P("ep", None, "tp"),
        P("ep", None, "tp"),
        P("ep", "tp", None),
        P(None, "tp"),
        P(None, "tp"),
        P("tp", None),
    )
    return jax.shard_map(
        body, mesh=mesh, in_specs=placed, out_specs=P(("ep", "tp"), None), check_vma=False
    )
```

```python
import functools
import math

import jax
import jax.numpy as jnp
from jax import lax
from jax.experimental import pallas as pl
from jax.experimental.pallas import tpu as pltpu
from jax.sharding import PartitionSpec as P


epsilon = 1e-06
SPLIT = 12
SPARE = 6 * 1024 * 1024
BF16, F32 = jnp.bfloat16, jnp.float32


def dot(left, right):
    return jnp.dot(left, right, preferred_element_type=F32)


def call(kernel, outs, *args, lazy=0, scratch=(), flops=0):
    total, count = len(args), len(args) + len(outs)
    scalars = [a.dtype == jnp.int32 for a in args]
    moved = sum(a.size * a.dtype.itemsize for a in args)
    moved += sum(o.size * jnp.dtype(o.dtype).itemsize for o in outs)

    def wrapped(*refs):
        held, rest, sems = refs[:count], refs[count:-1], refs[-1]
        local = list(held)
        copies = {}
        for i in range(count):
            if i >= total or not scalars[i]:
                local[i], rest = rest[0], rest[1:]
            if i < total and not scalars[i]:
                copies[i] = pltpu.make_async_copy(held[i], local[i], sems.at[i])
                copies[i].start()
        for i in range(total - lazy):
            if i in copies:
                copies[i].wait()
        waits = [copies[i].wait for i in range(total - lazy, total)]
        kernel(*(waits and [waits]), *local, *rest)
        backs = [
            pltpu.make_async_copy(local[i], held[i], sems.at[i]) for i in range(total, count)
        ]
        for back in backs:
            back.start()
        for back in backs:
            back.wait()

    anywhere = pl.BlockSpec(memory_space=pltpu.HBM)
    in_specs = [pl.BlockSpec(memory_space=pltpu.SMEM) if s else anywhere for s in scalars]
    buffers = [pltpu.VMEM(a.shape, a.dtype) for a, s in zip(args, scalars) if not s]
    buffers += [pltpu.VMEM(o.shape, o.dtype) for o in outs]
    grant = SPARE + moved + sum(math.prod(b.shape) * b.dtype.itemsize for b in scratch)
    return pl.pallas_call(
        wrapped,
        out_shape=tuple([pltpu.HBM(o.shape, o.dtype) for o in outs]),
        in_specs=in_specs,
        out_specs=tuple([anywhere] * len(outs)),
        scratch_shapes=buffers + list(scratch) + [pltpu.SemaphoreType.DMA((count,))],
        compiler_params=pltpu.CompilerParams(vmem_limit_bytes=grant),
        cost_estimate=pl.CostEstimate(flops=flops, bytes_accessed=moved, transcendentals=0),
    )(
        *[
            a if s else pltpu.with_memory_space_constraint(a, pltpu.HBM)
            for a, s in zip(args, scalars)
        ]
    )


def array(shape, dtype=BF16):
    return jax.ShapeDtypeStruct(shape, dtype)


def norm_kernel(tokens_ref, gain_ref, normed_ref, *first_refs):
    values = tokens_ref[...].astype(F32)
    factor = lax.rsqrt(jnp.mean(values * values, axis=1, keepdims=True) + epsilon)
    normed = (values * factor * gain_ref[...]).astype(BF16)
    normed_ref[...] = normed
    for i, ref in enumerate(first_refs):
        ref[...] = normed[:, i * ref.shape[1] : (i + 1) * ref.shape[1]]


def ranks(member, axis):
    rows = member.shape[axis]
    one = lax.broadcasted_iota(jnp.int32, (rows, rows), 0)
    two = lax.broadcasted_iota(jnp.int32, (rows, rows), 1)
    flat = jnp.where(member, 1.0, 0.0).astype(BF16)
    if axis:
        count = dot(flat, jnp.where(one < two, 1.0, 0.0).astype(BF16))
    else:
        count = dot(jnp.where(two < one, 1.0, 0.0).astype(BF16), flat)
    return jnp.where(member, count, -1.0)


def slots_of(experts, cap, axis):
    shape = (experts * cap, experts) if axis == 0 else (experts, experts * cap)
    start = lax.broadcasted_iota(jnp.int32, shape, 1 - axis) * cap
    place = lax.broadcasted_iota(jnp.int32, shape, axis) - start
    inside = (place >= 0) & (place < cap)
    number = jnp.sum(jnp.where(inside, place, 0).astype(F32), axis=1 - axis, keepdims=True)
    return jnp.where(inside, 1.0, 0.0).astype(BF16), number


def picks(packet, me, experts, cap):
    numbers = (lax.broadcasted_iota(jnp.int32, (experts, 1), 0) ^ me).astype(F32)
    expand, place = slots_of(experts, cap, 0)
    member = (packet[0:1, :] == numbers) | (packet[1:2, :] == numbers)
    spread = dot(expand, ranks(member, 1).astype(BF16))
    return jnp.where(spread == place, 1.0, 0.0).astype(BF16)


def weighted(packet, me, experts, cap):
    rows = packet.shape[1]
    columns = jnp.concatenate([packet, jnp.zeros((128 - packet.shape[0], rows), F32)]).T
    numbers = (lax.broadcasted_iota(jnp.int32, (1, experts), 1) ^ me).astype(F32)
    expand, place = slots_of(experts, cap, 1)
    one, two = columns[:, 0:1] == numbers, columns[:, 1:2] == numbers
    spread = dot(ranks(one | two, 0).astype(BF16), expand)
    weight = jnp.where(one, columns[:, 2:3], 0.0) + jnp.where(two, columns[:, 3:4], 0.0)
    high = weight.astype(BF16)
    low = (weight - high.astype(F32)).astype(BF16)
    chosen = spread == place
    return [jnp.where(chosen, dot(part, expand), 0.0).astype(BF16) for part in (high, low)]


def put(refs, rows):
    size = refs[0].shape[0]
    for i, ref in enumerate(refs):
        ref[...] = rows[i * size : (i + 1) * size, :]


def gather(refs, into, row=0, column=0):
    size = refs[0].shape[0]
    for i, ref in enumerate(refs):
        start = row + i * size
        into[start : start + size, column : column + ref.shape[1]] = ref[...]


def put_all(ref, me, first, rows):
    if len(ref.shape) == 2:
        ref[first : first + rows.shape[0], :] = rows
        return
    size = ref.shape[1]
    for i in range(rows.shape[0] // size):
        ref[me ^ (first // size + i)] = rows[i * size : (i + 1) * size, :]


def gather_all(ref, me, first, into, columns):
    total = into.shape[0]
    if len(ref.shape) == 2:
        into[:, columns] = ref[first : first + total, :]
        return
    size = ref.shape[1]
    for i in range(total // size):
        into[i * size : (i + 1) * size, columns] = ref[me ^ (first // size + i)]


def send_kernel(experts, cap, me_ref, packet_ref, normed_ref, *outs):
    pick = picks(packet_ref[...], me_ref[0], experts, cap)
    near = experts // 2 * cap
    segments, plain_ref = outs[:-1], outs[-1]
    width = segments[0].shape[1]
    put(segments, dot(pick[:near], normed_ref[:, :width]).astype(BF16))
    put_all(plain_ref, me_ref[0], 0, dot(pick, normed_ref[:, width:]).astype(BF16))


def other_kernel(experts, cap, me_ref, packet_ref, block_ref, *outs):
    pick = picks(packet_ref[...], me_ref[0], experts, cap)
    put(outs, dot(pick, block_ref[...]).astype(BF16))


def ffn_kernel(count, waits, me_ref, *refs):
    near_in, refs = refs[:count], refs[count:]
    far_in, refs = (refs[:count], refs[count : 2 * count]), refs[2 * count :]
    plain_ref, weights, refs = refs[0], refs[1:7], refs[7:]
    near_out, far_out, refs = refs[:count], refs[count : 2 * count], refs[2 * count :]
    back_ref, rows_ref = refs
    near, model_width = rows_ref.shape[0] // 2, rows_ref.shape[1]
    width = near_in[0].shape[1]
    gather(near_in, rows_ref)
    for i, segments in enumerate(far_in):
        gather(segments, rows_ref, near, i * segments[0].shape[1])
    gather_all(plain_ref, me_ref[0], 0, rows_ref, slice(width, model_width))
    hidden = []
    for gate, up in ((0, 1), (2, 3)):
        waits[gate]()
        waits[up]()
        value = dot(rows_ref[...], weights[gate][...])
        value = value / (1.0 + jnp.exp(-value)) * dot(rows_ref[...], weights[up][...])
        hidden.append(value.astype(BF16))
    waits[4]()
    waits[5]()

    def down(rows, columns):
        return sum(dot(h[rows], weights[4 + i][:, columns]) for i, h in enumerate(hidden))

    for half, targets in enumerate((near_out, far_out)):
        rows = slice(half * near, (half + 1) * near)
        put(targets, down(rows, slice(0, width)).astype(BF16))
        rest = down(rows, slice(width, model_width)).astype(BF16)
        put_all(back_ref, me_ref[0], half * near, rest)


def partial_kernel(count, experts, cap, me_ref, packet_ref, *refs):
    masks = weighted(packet_ref[...], me_ref[0], experts, cap)
    segments, out_ref, rows_ref = refs[:count], refs[count], refs[count + 1]
    gather(segments, rows_ref)
    out_ref[...] = sum(dot(mask, rows_ref[...]) for mask in masks).astype(BF16)


def shared_kernel(waits, normed_ref, *refs):
    weights, out_ref = refs[:6], refs[6]
    normed = normed_ref[...]
    total = 0.0
    for gate, up, down in ((0, 1, 4), (2, 3, 5)):
        for w in (gate, up, down):
            waits[w]()
        value = dot(normed, weights[gate][...])
        hidden = value / (1.0 + jnp.exp(-value)) * dot(normed, weights[up][...])
        total = total + dot(hidden.astype(BF16), weights[down][...])
    out_ref[...] = total


def mine_kernel(count, experts, cap, me_ref, packet_ref, *refs):
    masks = weighted(packet_ref[...], me_ref[0], experts, cap)
    near = experts // 2 * cap
    segments, back_ref, shared_ref, out_ref, near_rows, all_rows = (
        refs[:count],
        *refs[count:],
    )
    gather(segments, near_rows)
    gather_all(back_ref, me_ref[0], 0, all_rows, slice(0, all_rows.shape[1]))
    split = near_rows.shape[1]
    one = sum(dot(mask[:, :near], near_rows[...]) for mask in masks)
    two = sum(dot(mask, all_rows[...]) for mask in masks)
    out_ref[:, :split] = shared_ref[:, :split] + one
    out_ref[:, split:] = shared_ref[:, split:] + two


def last_kernel(mine_ref, passed_ref, out_ref):
    split = passed_ref.shape[1]
    out_ref[:, :split] = (mine_ref[:, :split] + passed_ref[...].astype(F32)).astype(BF16)
    out_ref[:, split:] = mine_ref[:, split:].astype(BF16)


def swap_cores(array):
    size = lax.axis_size("tp")
    return lax.ppermute(array, "tp", [(i, (i + 1) % size) for i in range(size)])


def swap(array, bits):
    size = lax.axis_size("ep")
    return lax.ppermute(array, "ep", [(i, i ^ bits) for i in range(size)])


def exchange(segments):
    if len(segments) > 1:
        return [swap(segment, i) if i else segment for i, segment in enumerate(segments)]
    size = lax.axis_size("ep")
    half = size // 2
    rows = segments[0]
    order = jnp.arange(half) ^ (lax.axis_index("ep") % half)
    groups = [list(range(half)), list(range(half, size))]
    blocks = rows.reshape(half, rows.shape[0] // half, rows.shape[1])[order]
    blocks = lax.all_to_all(blocks, "ep", 0, 0, tiled=True, axis_index_groups=groups)
    return [blocks[order].reshape(rows.shape)]


def exchange_all(rows):
    size = lax.axis_size("ep")
    order = jnp.arange(size) ^ lax.axis_index("ep")
    flat = len(rows.shape) == 2
    blocks = rows.reshape(size, rows.shape[0] // size, rows.shape[1])[order] if flat else rows
    blocks = lax.all_to_all(blocks, "ep", 0, 0, tiled=True)
    return blocks[order].reshape(rows.shape) if flat else blocks


def body(
    tokens,
    norm_gain,
    expert_ids,
    route_weights,
    expert_gate,
    expert_up,
    expert_down,
    shared_gate,
    shared_up,
    shared_down,
):
    return layer(
        tokens,
        norm_gain,
        expert_ids,
        route_weights,
        (expert_gate[0], expert_up[0], expert_down[0]),
        (shared_gate, shared_up, shared_down),
    )


def both_halves(gate_w, up_w, down_w):
    gate_o, up_o = swap_cores(gate_w), swap_cores(up_w)
    return gate_w, up_w, gate_o, up_o, down_w, swap_cores(down_w)


def layer(tokens, norm_gain, expert_ids, route_weights, routed_w, shared_w):
    rows, model_width = tokens.shape
    ep_size = lax.axis_size("ep")
    half = ep_size // 2
    cap = 3 * rows * expert_ids.shape[1] // (2 * ep_size)
    width = model_width * SPLIT // 16
    rest = model_width - width
    near = half * cap
    count = half if half <= 8 else 1
    part = near // count
    hidden = 2 * routed_w[0].shape[1]

    me = lax.axis_index("ep").astype(jnp.int32)[None]
    plain_shape = (ep_size, cap, rest) if count > 1 else (ep_size * cap, rest)

    normed, *first = call(
        norm_kernel,
        [array((rows, model_width))] + [array((rows, width // 2))] * 2,
        tokens,
        norm_gain[None, :],
        flops=4 * rows * model_width,
    )
    mirrored = [swap(block, half) for block in first]
    packet = jnp.concatenate([expert_ids.T.astype(F32), route_weights.T])
    other_packet = swap(packet, half)
    *own, plain = call(
        functools.partial(send_kernel, ep_size, cap),
        [array((part, width))] * count + [array(plain_shape)],
        me,
        packet,
        normed,
        flops=2 * near * rows * (model_width + rest),
    )
    own_in = exchange(own)
    plain_in = exchange_all(plain)
    weights = both_halves(*routed_w)
    shared = both_halves(*shared_w)

    other_in = []
    for block in mirrored:
        other = call(
            functools.partial(other_kernel, half, cap),
            [array((part, width // 2))] * count,
            me,
            other_packet,
            block,
            flops=near * rows * width,
        )
        other_in += exchange(other)
    *done, plain_out = call(
        functools.partial(ffn_kernel, count),
        [array((part, width))] * (2 * count) + [array(plain_shape)],
        me,
        *own_in,
        *other_in,
        plain_in,
        *weights,
        lazy=6,
        scratch=[pltpu.VMEM((2 * near, model_width), BF16)],
        flops=12 * near * model_width * hidden,
    )
    plain_back = exchange_all(plain_out)
    other_back = exchange(done[count:])
    own_back = exchange(done[:count])
    (partial,) = call(
        functools.partial(partial_kernel, count, half, cap),
        [array((rows, width))],
        me,
        other_packet,
        *other_back,
        scratch=[pltpu.VMEM((near, width), BF16)],
        flops=4 * near * rows * width,
    )
    passed = swap(partial, half)
    (shared_out,) = call(
        shared_kernel,
        [array((rows, model_width), F32)],
        normed,
        *shared,
        lazy=6,
        flops=6 * rows * model_width * hidden,
    )
    (mine,) = call(
        functools.partial(mine_kernel, count, ep_size, cap),
        [array((rows, model_width), F32)],
        me,
        packet,
        *own_back,
        plain_back,
        shared_out,
        scratch=[pltpu.VMEM((near, width), BF16), pltpu.VMEM((2 * near, rest), BF16)],
        flops=4 * near * rows * (model_width + rest),
    )
    (out,) = call(last_kernel, [array((rows, model_width))], mine, passed, flops=rows * model_width)
    return out


def solution(mesh):
    placed = (
        P(("ep", "tp"), None),
        P(),
        P(("ep", "tp"), None),
        P(("ep", "tp"), None),
        P("ep", None, "tp"),
        P("ep", None, "tp"),
        P("ep", "tp", None),
        P(None, "tp"),
        P(None, "tp"),
        P("tp", None),
    )
    return jax.shard_map(
        body, mesh=mesh, in_specs=placed, out_specs=P(("ep", "tp"), None), check_vma=False
    )
```

```python
import functools
import math

import jax
import jax.numpy as jnp
from jax import lax
from jax.experimental import pallas as pl
from jax.experimental.pallas import tpu as pltpu
from jax.sharding import PartitionSpec as P


epsilon = 1e-06
SPLIT = 12
SPARE = 6 * 1024 * 1024
BF16, F32 = jnp.bfloat16, jnp.float32


def dot(left, right):
    return jnp.dot(left, right, preferred_element_type=F32)


def call(kernel, outs, *args, lazy=0, resident=0, keep=0, scratch=(), flops=0):
    total, count = len(args), len(args) + len(outs)
    scalars = [a.dtype == jnp.int32 for a in args]
    still = [s or i >= total - resident for i, s in enumerate(scalars)]
    still += [i >= len(outs) - keep for i in range(len(outs))]
    moved = sum(a.size * a.dtype.itemsize for a in args)
    moved += sum(o.size * jnp.dtype(o.dtype).itemsize for o in outs)

    def wrapped(*refs):
        held, rest, sems = refs[:count], refs[count:-1], refs[-1]
        local = list(held)
        copies = {}
        for i in range(count):
            if not still[i]:
                local[i], rest = rest[0], rest[1:]
            if i < total and not still[i]:
                copies[i] = pltpu.make_async_copy(held[i], local[i], sems.at[i])
                copies[i].start()
        for i in range(total - lazy):
            if i in copies:
                copies[i].wait()
        waits = [copies[i].wait for i in range(total - lazy, total)]
        kernel(*(waits and [waits]), *local, *rest)
        backs = [
            pltpu.make_async_copy(local[i], held[i], sems.at[i])
            for i in range(total, count)
            if not still[i]
        ]
        for back in backs:
            back.start()
        for back in backs:
            back.wait()

    anywhere = pl.BlockSpec(memory_space=pltpu.HBM)
    near, scalar = pl.BlockSpec(memory_space=pltpu.VMEM), pl.BlockSpec(memory_space=pltpu.SMEM)
    in_specs = [scalar if s else near if t else anywhere for s, t in zip(scalars, still)]
    buffers = [pltpu.VMEM(a.shape, a.dtype) for a, t in zip(args, still) if not t]
    buffers += [pltpu.VMEM(o.shape, o.dtype) for o, t in zip(outs, still[total:]) if not t]
    spaces = [pltpu.VMEM if t else pltpu.HBM for t in still[total:]]
    grant = SPARE + moved + sum(math.prod(b.shape) * b.dtype.itemsize for b in scratch)
    return pl.pallas_call(
        wrapped,
        out_shape=tuple([space(o.shape, o.dtype) for o, space in zip(outs, spaces)]),
        in_specs=in_specs,
        out_specs=tuple([near if t else anywhere for t in still[total:]]),
        scratch_shapes=buffers + list(scratch) + [pltpu.SemaphoreType.DMA((count,))],
        compiler_params=pltpu.CompilerParams(vmem_limit_bytes=grant),
        cost_estimate=pl.CostEstimate(flops=flops, bytes_accessed=moved, transcendentals=0),
    )(*[a if s else pltpu.with_memory_space_constraint(a, pltpu.HBM) for a, s in zip(args, still)])


def array(shape, dtype=BF16):
    return jax.ShapeDtypeStruct(shape, dtype)


def norm_kernel(tokens_ref, gain_ref, normed_ref, *first_refs):
    values = tokens_ref[...].astype(F32)
    factor = lax.rsqrt(jnp.mean(values * values, axis=1, keepdims=True) + epsilon)
    normed = (values * factor * gain_ref[...]).astype(BF16)
    normed_ref[...] = normed
    for i, ref in enumerate(first_refs):
        ref[...] = normed[:, i * ref.shape[1] : (i + 1) * ref.shape[1]]


def ranks(member, axis):
    rows = member.shape[axis]
    one = lax.broadcasted_iota(jnp.int32, (rows, rows), 0)
    two = lax.broadcasted_iota(jnp.int32, (rows, rows), 1)
    flat = jnp.where(member, 1.0, 0.0).astype(BF16)
    if axis:
        count = dot(flat, jnp.where(one < two, 1.0, 0.0).astype(BF16))
    else:
        count = dot(jnp.where(two < one, 1.0, 0.0).astype(BF16), flat)
    return jnp.where(member, count, -1.0)


def slots_of(experts, cap, axis):
    shape = (experts * cap, experts) if axis == 0 else (experts, experts * cap)
    start = lax.broadcasted_iota(jnp.int32, shape, 1 - axis) * cap
    place = lax.broadcasted_iota(jnp.int32, shape, axis) - start
    inside = (place >= 0) & (place < cap)
    number = jnp.sum(jnp.where(inside, place, 0).astype(F32), axis=1 - axis, keepdims=True)
    return jnp.where(inside, 1.0, 0.0).astype(BF16), number


def picks(packet, me, experts, cap):
    numbers = (lax.broadcasted_iota(jnp.int32, (experts, 1), 0) ^ me).astype(F32)
    expand, place = slots_of(experts, cap, 0)
    member = (packet[0:1, :] == numbers) | (packet[1:2, :] == numbers)
    spread = dot(expand, ranks(member, 1).astype(BF16))
    return jnp.where(spread == place, 1.0, 0.0).astype(BF16)


def weighted(packet, me, experts, cap):
    rows = packet.shape[1]
    columns = jnp.concatenate([packet, jnp.zeros((128 - packet.shape[0], rows), F32)]).T
    numbers = (lax.broadcasted_iota(jnp.int32, (1, experts), 1) ^ me).astype(F32)
    expand, place = slots_of(experts, cap, 1)
    one, two = columns[:, 0:1] == numbers, columns[:, 1:2] == numbers
    spread = dot(ranks(one | two, 0).astype(BF16), expand)
    weight = jnp.where(one, columns[:, 2:3], 0.0) + jnp.where(two, columns[:, 3:4], 0.0)
    high = weight.astype(BF16)
    low = (weight - high.astype(F32)).astype(BF16)
    chosen = spread == place
    return [jnp.where(chosen, dot(part, expand), 0.0).astype(BF16) for part in (high, low)]


def put(refs, rows):
    size = refs[0].shape[0]
    for i, ref in enumerate(refs):
        ref[...] = rows[i * size : (i + 1) * size, :]


def gather(refs, into, row=0, column=0):
    size = refs[0].shape[0]
    for i, ref in enumerate(refs):
        start = row + i * size
        into[start : start + size, column : column + ref.shape[1]] = ref[...]


def put_all(ref, me, first, rows):
    if len(ref.shape) == 2:
        ref[first : first + rows.shape[0], :] = rows
        return
    size = ref.shape[1]
    for i in range(rows.shape[0] // size):
        ref[me ^ (first // size + i)] = rows[i * size : (i + 1) * size, :]


def gather_all(ref, me, first, into, columns):
    total = into.shape[0]
    if len(ref.shape) == 2:
        into[:, columns] = ref[first : first + total, :]
        return
    size = ref.shape[1]
    for i in range(total // size):
        into[i * size : (i + 1) * size, columns] = ref[me ^ (first // size + i)]


def send_kernel(experts, cap, me_ref, packet_ref, normed_ref, *outs):
    pick = picks(packet_ref[...], me_ref[0], experts, cap)
    near = experts // 2 * cap
    segments, plain_ref = outs[:-1], outs[-1]
    width = segments[0].shape[1]
    put(segments, dot(pick[:near], normed_ref[:, :width]).astype(BF16))
    put_all(plain_ref, me_ref[0], 0, dot(pick, normed_ref[:, width:]).astype(BF16))


def other_kernel(experts, cap, me_ref, packet_ref, block_ref, *outs):
    pick = picks(packet_ref[...], me_ref[0], experts, cap)
    put(outs, dot(pick, block_ref[...]).astype(BF16))


def ffn_kernel(count, waits, me_ref, *refs):
    near_in, refs = refs[:count], refs[count:]
    far_in, refs = (refs[:count], refs[count : 2 * count]), refs[2 * count :]
    plain_ref, weights, refs = refs[0], refs[1:7], refs[7:]
    near_out, far_out, refs = refs[:count], refs[count : 2 * count], refs[2 * count :]
    back_ref, rows_ref = refs
    near, model_width = rows_ref.shape[0] // 2, rows_ref.shape[1]
    width = near_in[0].shape[1]
    gather(near_in, rows_ref)
    for i, segments in enumerate(far_in):
        gather(segments, rows_ref, near, i * segments[0].shape[1])
    gather_all(plain_ref, me_ref[0], 0, rows_ref, slice(width, model_width))
    hidden = []
    for gate, up in ((0, 1), (2, 3)):
        waits[gate]()
        waits[up]()
        value = dot(rows_ref[...], weights[gate][...])
        value = value / (1.0 + jnp.exp(-value)) * dot(rows_ref[...], weights[up][...])
        hidden.append(value.astype(BF16))
    waits[4]()
    waits[5]()

    def down(rows, columns):
        left = jnp.concatenate([h[rows] for h in hidden], axis=1)
        return dot(left, jnp.concatenate([w[:, columns] for w in weights[4:6]], axis=0))

    for half, targets in enumerate((near_out, far_out)):
        rows = slice(half * near, (half + 1) * near)
        put(targets, down(rows, slice(0, width)).astype(BF16))
        rest = down(rows, slice(width, model_width)).astype(BF16)
        put_all(back_ref, me_ref[0], half * near, rest)


def masks_kernel(experts, cap, me_ref, packet_ref, high_ref, low_ref):
    high_ref[...], low_ref[...] = weighted(packet_ref[...], me_ref[0], experts, cap)


def partial_kernel(count, high_ref, low_ref, *refs):
    segments, out_ref, rows_ref = refs[:count], refs[count], refs[count + 1]
    gather(segments, rows_ref)
    rows = rows_ref[...]
    out_ref[...] = (dot(high_ref[...], rows) + dot(low_ref[...], rows)).astype(BF16)


def shared_kernel(waits, normed_ref, *refs):
    weights, out_ref = refs[:6], refs[6]
    normed = normed_ref[...]
    total = 0.0
    for gate, up, down in ((0, 1, 4), (2, 3, 5)):
        for w in (gate, up, down):
            waits[w]()
        value = dot(normed, weights[gate][...])
        hidden = value / (1.0 + jnp.exp(-value)) * dot(normed, weights[up][...])
        total = total + dot(hidden.astype(BF16), weights[down][...])
    out_ref[...] = total


def mine_kernel(count, experts, cap, me_ref, packet_ref, *refs):
    masks = weighted(packet_ref[...], me_ref[0], experts, cap)
    near = experts // 2 * cap
    segments, back_ref, shared_ref, out_ref, near_rows, all_rows = (
        refs[:count],
        *refs[count:],
    )
    gather(segments, near_rows)
    gather_all(back_ref, me_ref[0], 0, all_rows, slice(0, all_rows.shape[1]))
    split = near_rows.shape[1]
    one = sum(dot(mask[:, :near], near_rows[...]) for mask in masks)
    two = sum(dot(mask, all_rows[...]) for mask in masks)
    out_ref[:, :split] = shared_ref[:, :split] + one
    out_ref[:, split:] = shared_ref[:, split:] + two


def last_kernel(mine_ref, passed_ref, out_ref):
    split = passed_ref.shape[1]
    out_ref[:, :split] = (mine_ref[:, :split] + passed_ref[...].astype(F32)).astype(BF16)
    out_ref[:, split:] = mine_ref[:, split:].astype(BF16)


def swap_cores(array):
    size = lax.axis_size("tp")
    return lax.ppermute(array, "tp", [(i, (i + 1) % size) for i in range(size)])


def swap(array, bits):
    size = lax.axis_size("ep")
    return lax.ppermute(array, "ep", [(i, i ^ bits) for i in range(size)])


def exchange(segments):
    if len(segments) > 1:
        return [swap(segment, i) if i else segment for i, segment in enumerate(segments)]
    size = lax.axis_size("ep")
    half = size // 2
    rows = segments[0]
    order = jnp.arange(half) ^ (lax.axis_index("ep") % half)
    groups = [list(range(half)), list(range(half, size))]
    blocks = rows.reshape(half, rows.shape[0] // half, rows.shape[1])[order]
    blocks = lax.all_to_all(blocks, "ep", 0, 0, tiled=True, axis_index_groups=groups)
    return [blocks[order].reshape(rows.shape)]


def exchange_all(rows):
    size = lax.axis_size("ep")
    order = jnp.arange(size) ^ lax.axis_index("ep")
    flat = len(rows.shape) == 2
    blocks = rows.reshape(size, rows.shape[0] // size, rows.shape[1])[order] if flat else rows
    blocks = lax.all_to_all(blocks, "ep", 0, 0, tiled=True)
    return blocks[order].reshape(rows.shape) if flat else blocks


def body(
    tokens,
    norm_gain,
    expert_ids,
    route_weights,
    expert_gate,
    expert_up,
    expert_down,
    shared_gate,
    shared_up,
    shared_down,
):
    return layer(
        tokens,
        norm_gain,
        expert_ids,
        route_weights,
        (expert_gate[0], expert_up[0], expert_down[0]),
        (shared_gate, shared_up, shared_down),
    )


def both_halves(gate_w, up_w, down_w):
    gate_o, up_o = swap_cores(gate_w), swap_cores(up_w)
    return gate_w, up_w, gate_o, up_o, down_w, swap_cores(down_w)


def layer(tokens, norm_gain, expert_ids, route_weights, routed_w, shared_w):
    rows, model_width = tokens.shape
    ep_size = lax.axis_size("ep")
    half = ep_size // 2
    cap = 3 * rows * expert_ids.shape[1] // (2 * ep_size)
    width = model_width * SPLIT // 16
    rest = model_width - width
    near = half * cap
    count = half if half <= 8 else 1
    part = near // count
    hidden = 2 * routed_w[0].shape[1]

    me = lax.axis_index("ep").astype(jnp.int32)[None]
    plain_shape = (ep_size, cap, rest) if count > 1 else (ep_size * cap, rest)

    normed, *first = call(
        norm_kernel,
        [array((rows, model_width))] + [array((rows, width // 2))] * 2,
        tokens,
        norm_gain[None, :],
        flops=4 * rows * model_width,
    )
    mirrored = [swap(block, half) for block in first]
    packet = jnp.concatenate([expert_ids.T.astype(F32), route_weights.T])
    other_packet = swap(packet, half)
    *own, plain = call(
        functools.partial(send_kernel, ep_size, cap),
        [array((part, width))] * count + [array(plain_shape)],
        me,
        packet,
        normed,
        flops=2 * near * rows * (model_width + rest),
    )
    own_in = exchange(own)
    plain_in = exchange_all(plain)
    weights = both_halves(*routed_w)
    shared = both_halves(*shared_w)

    other_in = []
    for block in mirrored:
        other = call(
            functools.partial(other_kernel, half, cap),
            [array((part, width // 2))] * count,
            me,
            other_packet,
            block,
            resident=1,
            flops=near * rows * width,
        )
        other_in += exchange(other)
    masks = call(
        functools.partial(masks_kernel, half, cap),
        [array((rows, near))] * 2,
        me,
        other_packet,
        flops=rows * rows * near,
    )
    *done, plain_out = call(
        functools.partial(ffn_kernel, count),
        [array((part, width))] * (2 * count) + [array(plain_shape)],
        me,
        *own_in,
        *other_in,
        plain_in,
        *weights,
        lazy=6,
        scratch=[pltpu.VMEM((2 * near, model_width), BF16)],
        flops=12 * near * model_width * hidden,
    )
    plain_back = exchange_all(plain_out)
    other_back = exchange(done[count:])
    own_back = exchange(done[:count])
    (partial,) = call(
        functools.partial(partial_kernel, count),
        [array((rows, width))],
        *masks,
        *other_back,
        scratch=[pltpu.VMEM((near, width), BF16)],
        flops=4 * near * rows * width,
    )
    passed = swap(partial, half)
    (shared_out,) = call(
        shared_kernel,
        [array((rows, model_width), F32)],
        normed,
        *shared,
        lazy=6,
        flops=6 * rows * model_width * hidden,
    )
    (mine,) = call(
        functools.partial(mine_kernel, count, ep_size, cap),
        [array((rows, model_width), F32)],
        me,
        packet,
        *own_back,
        plain_back,
        shared_out,
        scratch=[pltpu.VMEM((near, width), BF16), pltpu.VMEM((2 * near, rest), BF16)],
        flops=4 * near * rows * (model_width + rest),
        keep=1,
    )
    (out,) = call(
        last_kernel,
        [array((rows, model_width))],
        mine,
        passed,
        resident=2,
        flops=rows * model_width,
    )
    return out


def solution(mesh):
    placed = (
        P(("ep", "tp"), None),
        P(),
        P(("ep", "tp"), None),
        P(("ep", "tp"), None),
        P("ep", None, "tp"),
        P("ep", None, "tp"),
        P("ep", "tp", None),
        P(None, "tp"),
        P(None, "tp"),
        P("tp", None),
    )
    return jax.shard_map(
        body, mesh=mesh, in_specs=placed, out_specs=P(("ep", "tp"), None), check_vma=False
    )
```
